32 devices in a mesh: grp: 2 (over y), fs: 4 (over z), tp: 4 (over x, core).
Axes of the slice: x: 2, y: 2, z: 4, core: 2. Of those that a mesh axis runs over, the one named last changes fastest.
Arguments:
- incoming_representations: bfloat16 [5120, 2048], P(('grp', 'fs', 'tp')), parts along dimension 0, may hold values from -6 to 6
- perceptron_switch_coefficients: bfloat16 [2048, 5120], P('fs', 'tp'), may hold values from -0.125 to 0.125
- perceptron_expand_coefficients: bfloat16 [2048, 5120], P('fs', 'tp'), may hold values from -0.125 to 0.125
- perceptron_contract_coefficients: bfloat16 [5120, 2048], P('tp', 'fs'), may hold values from -0.5 to 0.5
- probe_coefficients: bfloat16 [2048, 512], P('fs', 'tp'), may hold values from -0.125 to 0.125
- address_coefficients: bfloat16 [2048, 512], P('fs', 'tp'), may hold values from -0.125 to 0.125
- payload_coefficients: bfloat16 [2048, 1024], P('fs', 'tp'), may hold values from -0.125 to 0.125
- emit_switch_coefficients: bfloat16 [2048, 1024], P('fs', 'tp'), may hold values from -0.125 to 0.125
- forgetting_shrink_coefficients: bfloat16 [2048, 32], replicated, may hold values from -0.125 to 0.125
- forgetting_expand_coefficients: bfloat16 [32, 512], P(None, 'tp'), may hold values from -3 to 3
- forgetting_sigmoid_intercept: float32 [512], P('tp'), may hold values from -1 to 9
- extra_forgetting_logits: float32 [5120, 512], P(('grp', 'fs'), 'tp'), parts along dimension 0, may hold values from -0.7 to 0
- subspace_rescaling_amplitude: float32 [128], replicated, may hold values from 0.1 to 1.9
- recurrence_emit_coefficients: bfloat16 [1024, 2048], P('tp', 'fs'), may hold values from -0.5 to 0.5
Outputs:
- layer_out: bfloat16 [5120, 2048], P(('grp', 'fs', 'tp')), parts along dimension 0
The draws below stay inside these ranges and needn't reach their ends.
There are 2 independent parts, one for each index of `grp`. The reference program is written for one: setup_inputs(seed, part) draws one part's arguments, and reference() takes and returns one part's arrays. A program takes and returns all parts, laid end to end along the dimension named above; an argument that names none is the same for every part. Nothing has to cross between parts.
All inputs are finite; a program needn't handle non-finite values.
Results may differ from the reference program's by a relative error of at most 0.035.
Values may be sent and summed in bfloat16 or wider, within the bound.
A program may use at most 64 MiB of HBM per device.

```python
import math
import jax
import jax.numpy as jnp
from jax import lax

D = 2048
FF = 5120
HEADS = 8
DK = 64
DV = 128
RANK = 32
BLOCK = 64
SEQUENCE_LENGTH = 320
TOKEN_TOTAL = 2560
N_TP = 4


def draw_forgetting_sigmoid_intercept(key, part):
    channels = HEADS * DK
    sequence_streams = jax.random.split(jax.random.fold_in(key, 7), 3)
    percent = 50
    chosen = (jax.random.randint(sequence_streams[0], (channels,), 0, 100) < percent).astype(jnp.float32)
    fast_bias = jax.random.uniform(sequence_streams[1], (channels,), jnp.float32, -1.0, 0.8)
    slow_bias = jax.random.uniform(sequence_streams[2], (channels,), jnp.float32, 5.0, 9.0)
    return chosen * fast_bias + (1.0 - chosen) * slow_bias


def draw_extra_forgetting_logits(key, part):
    channels = HEADS * DK
    sequence_streams = jax.random.split(jax.random.fold_in(key, 11), 4)
    sequence_total = TOKEN_TOTAL // SEQUENCE_LENGTH
    spike_first = jax.random.randint(sequence_streams[0], (sequence_total, 1), 0, SEQUENCE_LENGTH)
    spike_second = jax.random.randint(sequence_streams[1], (sequence_total, 1), 0, SEQUENCE_LENGTH)
    token_positions = jnp.arange(SEQUENCE_LENGTH)[None, :]
    spike_mask = ((token_positions == spike_first) | (token_positions == spike_second)).astype(jnp.float32).reshape(TOKEN_TOTAL, 1)
    spike_strength = jax.random.uniform(sequence_streams[2], (TOKEN_TOTAL, channels), jnp.float32, 0.22, 0.69)
    block_total = TOKEN_TOTAL // BLOCK
    decay_offset_term = jnp.exp(jax.random.uniform(sequence_streams[3], (block_total, 1, channels), jnp.float32, math.log(0.0002), math.log(0.003)))
    decay_offset_term = jnp.broadcast_to(decay_offset_term, (block_total, BLOCK, channels)).reshape(TOKEN_TOTAL, channels)
    return -(spike_mask * spike_strength + decay_offset_term)


def block_scale(own_key, shape, pieces, low, largest):
    gain = 1.0
    for position, parts in pieces:
        heights = jax.random.uniform(jax.random.fold_in(jax.random.fold_in(own_key, 6), position), (parts,), jnp.float32, low / len(pieces), largest / len(pieces))
        gain = gain * jnp.repeat(jnp.exp(heights), shape[position] // parts).reshape((-1,) + (1,) * (len(shape) - 1 - position))
    return gain


def bell_draw(stream_key, shape, width, limit, pieces=(), kind=jnp.bfloat16):
    loudness = block_scale(stream_key, shape, pieces, -0.22, 0.18) if pieces else 1.0
    values = jax.random.normal(stream_key, shape, jnp.float32) * width * loudness
    return jnp.minimum(jnp.maximum(values, -limit), limit).astype(kind)


def setup_inputs(seed: int = 0, part: int = 0) -> dict:
    seeds = jax.random.split(jax.random.key(seed), 15)
    part_splits = jax.random.split(jax.random.fold_in(seeds[14], part), 15)
    return {
        "incoming_representations": bell_draw(part_splits[0], (TOKEN_TOTAL, D), 1.0, 6.0, ((0, 16),)),
        "perceptron_switch_coefficients": bell_draw(seeds[1], (D, FF), D ** -0.5, 0.125, ((0, 4), (1, 4))),
        "perceptron_expand_coefficients": bell_draw(seeds[2], (D, FF), D ** -0.5, 0.125, ((0, 4), (1, 4))),
        "perceptron_contract_coefficients": bell_draw(seeds[3], (FF, D), (max(FF // 36, 1)) ** -0.5, 0.5, ((0, 4), (1, 4))),
        "probe_coefficients": bell_draw(seeds[4], (D, HEADS * DK), D ** -0.5, 0.125, ((0, 4), (1, 4))),
        "address_coefficients": bell_draw(seeds[5], (D, HEADS * DK), D ** -0.5, 0.125, ((0, 4), (1, 4))),
        "payload_coefficients": bell_draw(seeds[6], (D, HEADS * DV), D ** -0.5, 0.125, ((0, 4), (1, 4))),
        "emit_switch_coefficients": bell_draw(seeds[7], (D, HEADS * DV), D ** -0.5, 0.125, ((0, 4), (1, 4))),
        "forgetting_shrink_coefficients": bell_draw(seeds[8], (D, RANK), D ** -0.5, 0.125),
        "forgetting_expand_coefficients": bell_draw(seeds[9], (RANK, HEADS * DK), (3 * RANK ** -0.5), 3.0, ((1, 4),)),
        "forgetting_sigmoid_intercept": draw_forgetting_sigmoid_intercept(jax.random.fold_in(seeds[14], 71), part),
        "extra_forgetting_logits": draw_extra_forgetting_logits(jax.random.fold_in(jax.random.fold_in(seeds[14], part), 71), part),
        "subspace_rescaling_amplitude": jnp.clip(1.0 + 0.18 * jax.random.normal(seeds[12], (DV,), jnp.float32), 0.1, 1.9),
        "recurrence_emit_coefficients": bell_draw(seeds[13], (HEADS * DV, D), (max(HEADS * DV // 9, 1)) ** -0.5, 0.5, ((0, 4), (1, 4))),
    }


residual_gain = 1.681792830507429
forgetting_steepness_multiplier = 16.0
epsilon = 1e-06
highest = lax.Precision.HIGHEST

def post_norm(residual, branch):
    summed = residual_gain * residual.astype(jnp.float32) + branch
    average = lax.optimization_barrier(jnp.mean(summed, axis=-1, keepdims=True))
    centred = summed - average
    variance = lax.optimization_barrier(jnp.mean(centred * centred, axis=-1, keepdims=True))
    return (centred * lax.rsqrt(variance + epsilon)).astype(jnp.bfloat16)

def rounded_sum(hidden, weight):
    block_width = hidden.shape[1] // N_TP
    totals = jnp.zeros((hidden.shape[0], weight.shape[1]), jnp.float32)
    for block_index in range(N_TP):
        begin = block_index * block_width
        partial_value = jnp.dot(hidden[:, begin:begin + block_width], weight[begin:begin + block_width], preferred_element_type=jnp.float32)
        partial_value = lax.optimization_barrier(partial_value.astype(jnp.bfloat16))
        totals = totals + partial_value.astype(jnp.float32)
    return totals

def channel_half(latent_representations, perceptron_switch_coefficients, perceptron_expand_coefficients, perceptron_contract_coefficients):
    gate_sum = jnp.dot(latent_representations, perceptron_switch_coefficients, preferred_element_type=jnp.float32)
    up_sum = jnp.dot(latent_representations, perceptron_expand_coefficients, preferred_element_type=jnp.float32)
    hidden = (jax.nn.silu(gate_sum) * up_sum).astype(jnp.bfloat16)
    return post_norm(latent_representations, 0.5 * rounded_sum(hidden, perceptron_contract_coefficients))

def linear_attention(queries, key_rows, values, forgetting_euler_power):
    token_count = queries.shape[0]
    seq_count = token_count // SEQUENCE_LENGTH

    def by_position(source, channels):
        shaped = source.astype(jnp.float32).reshape(seq_count, SEQUENCE_LENGTH, HEADS, channels)
        return shaped.transpose(1, 0, 2, 3)
    inputs = (by_position(queries, DK), by_position(key_rows, DK), by_position(values, DV), jnp.exp(by_position(forgetting_euler_power, DK)))
    start_state = jnp.zeros((seq_count, HEADS, DK, DV), jnp.float32)

    def forward(carried, step_in):
        query_now, key_now, value_now, decay_now = step_in
        carried = decay_now[..., None] * carried + key_now[..., None] * value_now[..., None, :]
        return (carried, jnp.einsum('shd,shdv->shv', query_now, carried, precision=highest))

    def reverse_direction_sweep(carried, step_in):
        query_now, key_now, value_now, decay_now = step_in
        seen = decay_now[..., None] * carried
        return (seen + key_now[..., None] * value_now[..., None, :], jnp.einsum('shd,shdv->shv', query_now, seen, precision=highest))
    _, from_before = lax.scan(forward, start_state, inputs)
    _, from_after = lax.scan(reverse_direction_sweep, start_state, inputs, reverse=True)
    return (from_before + from_after).transpose(1, 0, 2, 3).reshape(token_count, HEADS, DV)

def recurrent_context_blender(latent_representations, probe_coefficients, address_coefficients, payload_coefficients, emit_switch_coefficients, forgetting_shrink_coefficients, forgetting_expand_coefficients, forgetting_sigmoid_intercept, extra_forgetting_logits, subspace_rescaling_amplitude, recurrence_emit_coefficients):
    queries = jnp.dot(latent_representations, probe_coefficients, preferred_element_type=jnp.float32).astype(jnp.bfloat16)
    key_rows = jnp.dot(latent_representations, address_coefficients, preferred_element_type=jnp.float32).astype(jnp.bfloat16)
    values = jnp.dot(latent_representations, payload_coefficients, preferred_element_type=jnp.float32).astype(jnp.bfloat16)
    outgate = jnp.dot(latent_representations, emit_switch_coefficients, preferred_element_type=jnp.float32).astype(jnp.bfloat16)
    compact_inner_dimensionality = jnp.dot(latent_representations, forgetting_shrink_coefficients, preferred_element_type=jnp.float32).astype(jnp.bfloat16)
    forgetting_euler_power = jax.nn.log_sigmoid(jnp.dot(compact_inner_dimensionality, forgetting_expand_coefficients, preferred_element_type=jnp.float32) + forgetting_sigmoid_intercept) / forgetting_steepness_multiplier + extra_forgetting_logits
    mixed_heads = linear_attention(queries, key_rows, values, forgetting_euler_power)
    scaled = mixed_heads * lax.rsqrt(lax.optimization_barrier(jnp.mean(mixed_heads * mixed_heads, axis=-1, keepdims=True)) + epsilon) * subspace_rescaling_amplitude
    opener = jax.nn.silu(outgate.astype(jnp.float32)).reshape(mixed_heads.shape)
    gated = (scaled * opener).reshape(mixed_heads.shape[0], HEADS * DV).astype(jnp.bfloat16)
    return post_norm(latent_representations, rounded_sum(gated, recurrence_emit_coefficients))

def reference(incoming_representations, perceptron_switch_coefficients, perceptron_expand_coefficients, perceptron_contract_coefficients, probe_coefficients, address_coefficients, payload_coefficients, emit_switch_coefficients, forgetting_shrink_coefficients, forgetting_expand_coefficients, forgetting_sigmoid_intercept, extra_forgetting_logits, subspace_rescaling_amplitude, recurrence_emit_coefficients):
    opening_perceptron_result = channel_half(incoming_representations, perceptron_switch_coefficients, perceptron_expand_coefficients, perceptron_contract_coefficients)
    context_blend_result = recurrent_context_blender(opening_perceptron_result, probe_coefficients, address_coefficients, payload_coefficients, emit_switch_coefficients, forgetting_shrink_coefficients, forgetting_expand_coefficients, forgetting_sigmoid_intercept, extra_forgetting_logits, subspace_rescaling_amplitude, recurrence_emit_coefficients)
    return channel_half(context_blend_result, perceptron_switch_coefficients, perceptron_expand_coefficients, perceptron_contract_coefficients)
```

```python
import jax
import jax.numpy as jnp
from jax import lax
from jax.experimental import pallas as pl
from jax.experimental.pallas import tpu as pltpu
from jax.sharding import PartitionSpec as P

DK = 64
DV = 128
SEQUENCE_LENGTH = 320


residual_gain = 1.681792830507429
forgetting_steepness_multiplier = 16.0
epsilon = 1e-06


def post_norm(residual, branch):
    summed = residual_gain * residual.astype(jnp.float32) + branch
    average = jnp.mean(summed, axis=-1, keepdims=True)
    centred = summed - average
    variance = jnp.mean(centred * centred, axis=-1, keepdims=True)
    return (centred * lax.rsqrt(variance + epsilon)).astype(jnp.bfloat16)


def gather_group(stored):
    return lax.all_gather(stored, "tp", axis=0, tiled=True)


def after(value, earlier):
    return lax.optimization_barrier((value, earlier))[0]


def split_gather(stored, earlier=None):
    fs_count = lax.axis_size("fs")
    grp_count = lax.axis_size("grp")
    half_rows = stored.shape[0] // grp_count
    grp = lax.axis_index("grp")
    mine = lax.dynamic_slice_in_dim(stored, grp * half_rows, half_rows, 0)
    if earlier is not None:
        mine = after(mine, earlier)
    stacked = lax.all_gather(mine, "fs", axis=0, tiled=False)
    fs = lax.axis_index("fs")
    remote = jnp.stack(
        [
            lax.dynamic_index_in_dim(stacked, lax.rem(fs + step, fs_count), 0, keepdims=False)
            for step in range(1, fs_count)
        ]
    )
    swapped = lax.ppermute(remote, "grp", [(g, (g + 1) % grp_count) for g in range(grp_count)])
    return remote, swapped


def rotated_columns(gathered):
    fs_count = lax.axis_size("fs")
    grp_count = lax.axis_size("grp")
    width = gathered.shape[1] // fs_count
    half = width // grp_count
    fs = lax.axis_index("fs")
    grp = lax.axis_index("grp")
    own = lax.dynamic_slice_in_dim(gathered, fs * width, width, 1)

    def halves(which):
        return jnp.concatenate(
            [
                lax.dynamic_slice_in_dim(
                    gathered, lax.rem(fs + step, fs_count) * width + which * half, half, 1
                )
                for step in range(1, fs_count)
            ],
            axis=1,
        )

    return own, halves(grp), halves(grp_count - 1 - grp)


def project(columns, stored, fetched):
    own, mine, other = columns
    remote, swapped = fetched
    flat = (-1, stored.shape[1])
    return (
        jnp.dot(own, stored, preferred_element_type=jnp.float32)
        + jnp.dot(mine, remote.reshape(flat), preferred_element_type=jnp.float32)
        + jnp.dot(other, swapped.reshape(flat), preferred_element_type=jnp.float32)
    )


def scatter_rows(partial):
    return lax.psum_scatter(partial, "tp", scatter_dimension=0, tiled=True)


def contract(hidden, stored, fetched, earlier):
    fs_count = lax.axis_size("fs")
    grp_count = lax.axis_size("grp")
    remote, swapped = fetched
    width = stored.shape[1]
    half = hidden.shape[1] // grp_count
    grp = lax.axis_index("grp")
    mine = lax.dynamic_slice_in_dim(hidden, grp * half, half, 1)
    other = lax.dynamic_slice_in_dim(hidden, (grp_count - 1 - grp) * half, half, 1)
    pieces = [jnp.dot(hidden, stored, preferred_element_type=jnp.float32).astype(jnp.bfloat16)]
    for step in range(fs_count - 1):
        pieces.append(
            (
                jnp.dot(mine, remote[step], preferred_element_type=jnp.float32)
                + jnp.dot(other, swapped[step], preferred_element_type=jnp.float32)
            ).astype(jnp.bfloat16)
        )
    partial = jnp.concatenate(pieces, axis=1)
    if earlier is not None:
        partial = after(partial, earlier)
    summed = scatter_rows(partial)
    fs = lax.axis_index("fs")
    ordered = [
        lax.dynamic_slice_in_dim(
            summed, lax.rem(block - fs + fs_count, fs_count) * width, width, 1
        )
        for block in range(fs_count)
    ]
    return jnp.concatenate(ordered, axis=1).astype(jnp.float32)


def mixing_kernel(head_count, projected_ref, decay_ref, gain_ref, gated_ref):
    length = projected_ref.shape[0]
    key_width = head_count * DK
    value_width = head_count * DV
    queries = projected_ref[:, :key_width].astype(jnp.float32)
    key_rows = projected_ref[:, key_width : 2 * key_width].astype(jnp.float32)
    decay = decay_ref[...]
    rows = lax.broadcasted_iota(jnp.int32, (length, length), 0)
    columns = lax.broadcasted_iota(jnp.int32, (length, length), 1)
    apart = rows ^ columns
    channel = lax.broadcasted_iota(jnp.int32, (length, key_width), 1)
    top = decay.astype(jnp.bfloat16)
    rest = decay - top.astype(jnp.float32)
    middle = rest.astype(jnp.bfloat16)
    low = (rest - middle.astype(jnp.float32)).astype(jnp.bfloat16)

    def products(query_side, key_side):
        query_side = query_side.astype(jnp.bfloat16)
        found = []
        for head in range(head_count):
            inside = (channel >= head * DK) & (channel < (head + 1) * DK)
            one = jnp.where(inside, key_side, 0.0).astype(jnp.bfloat16)
            found.append(
                lax.dot_general(
                    query_side, one, (((1,), (1,)), ((), ())), preferred_element_type=jnp.float32
                )
            )
        return found

    scores = products(queries, key_rows)
    half = 1
    while half < length:
        level = half.bit_length() - 1
        upper = (rows & half) != 0
        reach = ((rows >> level) == (columns >> level)) & (
            (upper & (columns <= rows)) | (jnp.logical_not(upper) & (columns >= rows))
        )
        reach = jnp.where(reach, 1.0, 0.0).astype(jnp.bfloat16)
        through = (
            jnp.dot(reach, top, preferred_element_type=jnp.float32)
            + jnp.dot(reach, middle, preferred_element_type=jnp.float32)
            + jnp.dot(reach, low, preferred_element_type=jnp.float32)
        )
        before = jnp.minimum(through - decay, 0.0)
        found = products(queries * jnp.exp(through), key_rows * jnp.exp(before))
        scores = [jnp.where(apart >= half, new, old) for new, old in zip(found, scores)]
        half *= 2
    for head in range(head_count):
        begin = 2 * key_width + head * DV
        values = projected_ref[:, begin : begin + DV]
        mixed = jnp.dot(
            scores[head].astype(jnp.bfloat16), values, preferred_element_type=jnp.float32
        )
        begin += value_width
        opener = projected_ref[:, begin : begin + DV].astype(jnp.float32)
        scaled = (
            mixed
            * lax.rsqrt(jnp.mean(mixed * mixed, axis=-1, keepdims=True) + epsilon)
            * gain_ref[...]
        )
        gated_ref[:, head * DV : (head + 1) * DV] = (
            scaled * (opener / (1.0 + jnp.exp(-opener)))
        ).astype(jnp.bfloat16)


def mix(projected, decay, gain):
    tokens, key_width = decay.shape
    head_count = key_width // DK
    seq_count = tokens // SEQUENCE_LENGTH

    def block(width):
        return pl.BlockSpec((SEQUENCE_LENGTH, width), lambda seq: (seq, 0))

    return pl.pallas_call(
        lambda *refs: mixing_kernel(head_count, *refs),
        out_shape=jax.ShapeDtypeStruct((tokens, head_count * DV), jnp.bfloat16),
        grid=(seq_count,),
        in_specs=[
            block(projected.shape[1]),
            block(key_width),
            pl.BlockSpec((1, DV), lambda seq: (0, 0)),
        ],
        out_specs=block(head_count * DV),
        name="mixing",
        cost_estimate=pl.CostEstimate(
            flops=4000000 * tokens, bytes_accessed=4000 * tokens, transcendentals=3000 * tokens
        ),
    )(projected, decay, gain.reshape(1, DV))


def per_device(
    incoming_representations,
    perceptron_switch_coefficients,
    perceptron_expand_coefficients,
    perceptron_contract_coefficients,
    probe_coefficients,
    address_coefficients,
    payload_coefficients,
    emit_switch_coefficients,
    forgetting_shrink_coefficients,
    forgetting_expand_coefficients,
    forgetting_sigmoid_intercept,
    extra_forgetting_logits,
    subspace_rescaling_amplitude,
    recurrence_emit_coefficients,
):
    gate_weight = split_gather(perceptron_switch_coefficients)
    up_weight = split_gather(perceptron_expand_coefficients, gate_weight[0])
    down_weight = split_gather(perceptron_contract_coefficients, up_weight[0])
    mixer_stored = jnp.concatenate(
        [
            probe_coefficients,
            address_coefficients,
            payload_coefficients,
            emit_switch_coefficients,
        ],
        axis=1,
    )
    mixer_weight = split_gather(mixer_stored, down_weight[0])
    out_full = lax.all_gather(recurrence_emit_coefficients, "fs", axis=1, tiled=True)

    def channel_half(stored, entry, earlier):
        columns = rotated_columns(gather_group(entry))
        gate_sum = project(columns, perceptron_switch_coefficients, gate_weight)
        up_sum = project(columns, perceptron_expand_coefficients, up_weight)
        hidden = (jax.nn.silu(gate_sum) * up_sum).astype(jnp.bfloat16)
        return post_norm(
            stored, 0.5 * contract(hidden, perceptron_contract_coefficients, down_weight, earlier)
        )

    opening_perceptron_result = channel_half(
        incoming_representations,
        after(incoming_representations, up_weight[0]),
        mixer_weight[0],
    )
    gathered = gather_group(opening_perceptron_result)
    projected = project(rotated_columns(gathered), mixer_stored, mixer_weight).astype(
        jnp.bfloat16
    )
    compact_inner_dimensionality = jnp.dot(
        gathered, forgetting_shrink_coefficients, preferred_element_type=jnp.float32
    ).astype(jnp.bfloat16)
    forgetting_euler_power = (
        jax.nn.log_sigmoid(
            jnp.dot(
                compact_inner_dimensionality,
                forgetting_expand_coefficients,
                preferred_element_type=jnp.float32,
            )
            + forgetting_sigmoid_intercept
        )
        / forgetting_steepness_multiplier
        + extra_forgetting_logits
    )
    gated = mix(projected, forgetting_euler_power, subspace_rescaling_amplitude)
    branch = scatter_rows(
        jnp.dot(gated, out_full, preferred_element_type=jnp.float32).astype(jnp.bfloat16)
    ).astype(jnp.float32)
    context_blend_result = post_norm(opening_perceptron_result, branch)
    return channel_half(context_blend_result, context_blend_result, None)


def solution(mesh):
    return jax.shard_map(
        per_device,
        mesh=mesh,
        in_specs=(
            P(("grp", "fs", "tp"), None),
            P("fs", "tp"),
            P("fs", "tp"),
            P("tp", "fs"),
            P("fs", "tp"),
            P("fs", "tp"),
            P("fs", "tp"),
            P("fs", "tp"),
            P(),
            P(None, "tp"),
            P("tp"),
            P(("grp", "fs"), "tp"),
            P(),
            P("tp", "fs"),
        ),
        out_specs=P(("grp", "fs", "tp"), None),
        check_vma=False,
    )
```

```python
import jax
import jax.numpy as jnp
from jax import lax
from jax.experimental import pallas as pl
from jax.sharding import PartitionSpec as P

DK = 64
DV = 128
SEQUENCE_LENGTH = 320


residual_gain = 1.681792830507429
forgetting_steepness_multiplier = 16.0
epsilon = 1e-06


def post_norm(residual, branch):
    summed = residual_gain * residual.astype(jnp.float32) + branch
    average = jnp.mean(summed, axis=-1, keepdims=True)
    centred = summed - average
    variance = jnp.mean(centred * centred, axis=-1, keepdims=True)
    return (centred * lax.rsqrt(variance + epsilon)).astype(jnp.bfloat16)


def gather_group(stored):
    return lax.all_gather(stored, "tp", axis=0, tiled=True)


def after(value, earlier):
    return lax.optimization_barrier((value, earlier))[0]


def split_gather(stored, earlier=None):
    fs_count = lax.axis_size("fs")
    grp_count = lax.axis_size("grp")
    half_rows = stored.shape[0] // grp_count
    grp = lax.axis_index("grp")
    mine = lax.dynamic_slice_in_dim(stored, grp * half_rows, half_rows, 0)
    if earlier is not None:
        mine = after(mine, earlier)
    stacked = lax.all_gather(mine, "fs", axis=0, tiled=False)
    fs = lax.axis_index("fs")
    remote = jnp.stack(
        [
            lax.dynamic_index_in_dim(stacked, lax.rem(fs + step, fs_count), 0, keepdims=False)
            for step in range(1, fs_count)
        ]
    )
    swapped = lax.ppermute(
        remote, "grp", [(g, (g + 1) % grp_count) for g in range(grp_count)]
    )
    return remote, swapped


def rotated_columns(gathered):
    fs_count = lax.axis_size("fs")
    grp_count = lax.axis_size("grp")
    width = gathered.shape[1] // fs_count
    half = width // grp_count
    fs = lax.axis_index("fs")
    grp = lax.axis_index("grp")
    own = lax.dynamic_slice_in_dim(gathered, fs * width, width, 1)

    def halves(which):
        return jnp.concatenate(
            [
                lax.dynamic_slice_in_dim(
                    gathered, lax.rem(fs + step, fs_count) * width + which * half, half, 1
                )
                for step in range(1, fs_count)
            ],
            axis=1,
        )

    return own, halves(grp), halves(grp_count - 1 - grp)


def project(columns, stored, fetched):
    own, mine, other = columns
    remote, swapped = fetched
    flat = (-1, stored.shape[1])
    return (
        jnp.dot(own, stored, preferred_element_type=jnp.float32)
        + jnp.dot(mine, remote.reshape(flat), preferred_element_type=jnp.float32)
        + jnp.dot(other, swapped.reshape(flat), preferred_element_type=jnp.float32)
    )


def scatter_rows(partial):
    return lax.psum_scatter(partial, "tp", scatter_dimension=0, tiled=True)


def contract(hidden, stored, fetched, earlier):
    fs_count = lax.axis_size("fs")
    grp_count = lax.axis_size("grp")
    remote, swapped = fetched
    width = stored.shape[1]
    half = hidden.shape[1] // grp_count
    grp = lax.axis_index("grp")
    mine = lax.dynamic_slice_in_dim(hidden, grp * half, half, 1)
    other = lax.dynamic_slice_in_dim(hidden, (grp_count - 1 - grp) * half, half, 1)
    pieces = [jnp.dot(hidden, stored, preferred_element_type=jnp.float32).astype(jnp.bfloat16)]
    for step in range(fs_count - 1):
        pieces.append(
            (
                jnp.dot(mine, remote[step], preferred_element_type=jnp.float32)
                + jnp.dot(other, swapped[step], preferred_element_type=jnp.float32)
            ).astype(jnp.bfloat16)
        )
    partial = jnp.concatenate(pieces, axis=1)
    if earlier is not None:
        partial = after(partial, earlier)
    summed = scatter_rows(partial)
    fs = lax.axis_index("fs")
    ordered = [
        lax.dynamic_slice_in_dim(
            summed, lax.rem(block - fs + fs_count, fs_count) * width, width, 1
        )
        for block in range(fs_count)
    ]
    return jnp.concatenate(ordered, axis=1).astype(jnp.float32)


def mixing_kernel(head_count, projected_ref, decay_ref, gain_ref, gated_ref):
    length = projected_ref.shape[0]
    key_width = head_count * DK
    value_width = head_count * DV
    queries = projected_ref[:, :key_width].astype(jnp.float32)
    key_rows = projected_ref[:, key_width : 2 * key_width].astype(jnp.float32)
    decay = decay_ref[...]
    rows = lax.broadcasted_iota(jnp.int32, (length, length), 0)
    columns = lax.broadcasted_iota(jnp.int32, (length, length), 1)
    apart = rows ^ columns
    channel = lax.broadcasted_iota(jnp.int32, (length, key_width), 1)
    top = decay.astype(jnp.bfloat16)
    rest = decay - top.astype(jnp.float32)
    middle = rest.astype(jnp.bfloat16)
    low = (rest - middle.astype(jnp.float32)).astype(jnp.bfloat16)

    def products(query_side, key_side):
        query_side = query_side.astype(jnp.bfloat16)
        found = []
        for head in range(head_count):
            inside = (channel >= head * DK) & (channel < (head + 1) * DK)
            one = jnp.where(inside, key_side, 0.0).astype(jnp.bfloat16)
            found.append(
                lax.dot_general(
                    query_side, one, (((1,), (1,)), ((), ())), preferred_element_type=jnp.float32
                )
            )
        return found

    scores = products(queries, key_rows)
    half = 1
    while half < length:
        level = half.bit_length() - 1
        upper = (rows & half) != 0
        reach = ((rows >> level) == (columns >> level)) & (
            (upper & (columns <= rows)) | (jnp.logical_not(upper) & (columns >= rows))
        )
        reach = jnp.where(reach, 1.0, 0.0).astype(jnp.bfloat16)
        through = (
            jnp.dot(reach, top, preferred_element_type=jnp.float32)
            + jnp.dot(reach, middle, preferred_element_type=jnp.float32)
            + jnp.dot(reach, low, preferred_element_type=jnp.float32)
        )
        before = jnp.minimum(through - decay, 0.0)
        found = products(queries * jnp.exp(through), key_rows * jnp.exp(before))
        scores = [jnp.where(apart >= half, new, old) for new, old in zip(found, scores)]
        half *= 2
    for head in range(head_count):
        begin = 2 * key_width + head * DV
        values = projected_ref[:, begin : begin + DV]
        mixed = jnp.dot(
            scores[head].astype(jnp.bfloat16), values, preferred_element_type=jnp.float32
        )
        begin += value_width
        opener = projected_ref[:, begin : begin + DV].astype(jnp.float32)
        scaled = (
            mixed
            * lax.rsqrt(jnp.mean(mixed * mixed, axis=-1, keepdims=True) + epsilon)
            * gain_ref[...]
        )
        gated_ref[:, head * DV : (head + 1) * DV] = (
            scaled * (opener / (1.0 + jnp.exp(-opener)))
        ).astype(jnp.bfloat16)


def mix(projected, decay, gain):
    tokens, key_width = decay.shape
    head_count = key_width // DK
    seq_count = tokens // SEQUENCE_LENGTH

    def block(width):
        return pl.BlockSpec((SEQUENCE_LENGTH, width), lambda seq: (seq, 0))

    return pl.pallas_call(
        lambda *refs: mixing_kernel(head_count, *refs),
        out_shape=jax.ShapeDtypeStruct((tokens, head_count * DV), jnp.bfloat16),
        grid=(seq_count,),
        in_specs=[
            block(projected.shape[1]),
            block(key_width),
            pl.BlockSpec((1, DV), lambda seq: (0, 0)),
        ],
        out_specs=block(head_count * DV),
        name="mixing",
        cost_estimate=pl.CostEstimate(
            flops=4000000 * tokens, bytes_accessed=4000 * tokens, transcendentals=3000 * tokens
        ),
    )(projected, decay, gain.reshape(1, DV))


def per_device(
    incoming_representations,
    perceptron_switch_coefficients,
    perceptron_expand_coefficients,
    perceptron_contract_coefficients,
    probe_coefficients,
    address_coefficients,
    payload_coefficients,
    emit_switch_coefficients,
    forgetting_shrink_coefficients,
    forgetting_expand_coefficients,
    forgetting_sigmoid_intercept,
    extra_forgetting_logits,
    subspace_rescaling_amplitude,
    recurrence_emit_coefficients,
):
    gate_weight = split_gather(perceptron_switch_coefficients)
    up_weight = split_gather(perceptron_expand_coefficients, gate_weight[0])
    down_weight = split_gather(perceptron_contract_coefficients, up_weight[0])
    mixer_stored = jnp.concatenate(
        [
            probe_coefficients,
            address_coefficients,
            payload_coefficients,
            emit_switch_coefficients,
        ],
        axis=1,
    )
    mixer_weight = split_gather(mixer_stored, down_weight[0])
    out_full = lax.all_gather(recurrence_emit_coefficients, "fs", axis=1, tiled=True)

    def channel_half(stored, entry, earlier):
        gathered = gather_group(entry)
        columns = rotated_columns(gathered)
        gate_sum = project(columns, perceptron_switch_coefficients, gate_weight)
        up_sum = project(columns, perceptron_expand_coefficients, up_weight)
        hidden = (jax.nn.silu(gate_sum) * up_sum).astype(jnp.bfloat16)
        return post_norm(
            stored, 0.5 * contract(hidden, perceptron_contract_coefficients, down_weight, earlier)
        )

    opening_perceptron_result = channel_half(
        incoming_representations,
        after(incoming_representations, up_weight[0]),
        mixer_weight[0],
    )
    gathered = gather_group(opening_perceptron_result)
    projected = project(rotated_columns(gathered), mixer_stored, mixer_weight).astype(
        jnp.bfloat16
    )
    compact_inner_dimensionality = jnp.dot(
        gathered, forgetting_shrink_coefficients, preferred_element_type=jnp.float32
    ).astype(jnp.bfloat16)
    forgetting_euler_power = (
        jax.nn.log_sigmoid(
            jnp.dot(
                compact_inner_dimensionality,
                forgetting_expand_coefficients,
                preferred_element_type=jnp.float32,
            )
            + forgetting_sigmoid_intercept
        )
        / forgetting_steepness_multiplier
        + extra_forgetting_logits
    )
    gated = mix(projected, forgetting_euler_power, subspace_rescaling_amplitude)
    branch = scatter_rows(
        jnp.dot(gated, out_full, preferred_element_type=jnp.float32).astype(jnp.bfloat16)
    ).astype(jnp.float32)
    context_blend_result = post_norm(opening_perceptron_result, branch)
    return channel_half(context_blend_result, context_blend_result, None)


def solution(mesh):
    return jax.shard_map(
        per_device,
        mesh=mesh,
        in_specs=(
            P(("grp", "fs", "tp"), None),
            P("fs", "tp"),
            P("fs", "tp"),
            P("tp", "fs"),
            P("fs", "tp"),
            P("fs", "tp"),
            P("fs", "tp"),
            P("fs", "tp"),
            P(),
            P(None, "tp"),
            P("tp"),
            P(("grp", "fs"), "tp"),
            P(),
            P("tp", "fs"),
        ),
        out_specs=P(("grp", "fs", "tp"), None),
        check_vma=False,
    )
```
